32 devices in a mesh: sp: 4 (over z), fs: 4 (over y, x), tp: 2 (over core).
Axes of the slice: x: 2, y: 2, z: 4, core: 2. Of those that a mesh axis runs over, the one named last changes fastest.
Arguments:
- inputs: bfloat16 [4, 2048, 2048], P('fs', 'sp', 'tp'), may hold values from -6 to 6
- norm_gain: float32 [2048], replicated, may hold values from 0.1 to 1.9
- query_weight: bfloat16 [2048, 1024], P(('sp', 'fs'), 'tp'), may hold values from -0.125 to 0.125
- key_weight: bfloat16 [2048, 1024], P(('sp', 'fs'), 'tp'), may hold values from -0.125 to 0.125
- value_weight: bfloat16 [2048, 1024], P(('sp', 'fs'), 'tp'), may hold values from -0.125 to 0.125
- query_gain: float32 [64], replicated, may hold values from 0.8 to 7
- key_gain: float32 [64], replicated, may hold values from 0.8 to 7
- mix_lambda: float32 [8], replicated, may hold values from 0.3 to 0.8
- head_gain: float32 [128], replicated, may hold values from 0.1 to 1.9
- post_gate_weight: bfloat16 [2048, 2048], P(('sp', 'fs'), 'tp'), may hold values from -0.125 to 0.125
- pre_gate_weight: bfloat16 [2048, 2048], P(('sp', 'fs'), 'tp'), may hold values from -0.125 to 0.125
- inner_weight: bfloat16 [2048, 2048], P(('sp', 'fs'), 'tp'), may hold values from -0.125 to 0.125
- conv_taps: float32 [3, 2048], replicated, may hold values from -3 to 3
- attn_out_weight: bfloat16 [2048, 1024], P(('sp', 'fs'), 'tp'), may hold values from -0.109375 to 0.109375
- conv_out_weight: bfloat16 [2048, 2048], P(('sp', 'fs'), 'tp'), may hold values from -0.109375 to 0.109375
Outputs:
- mixed: bfloat16 [4, 2048, 2048], P('fs', ('sp', 'tp'))
The draws below stay inside these ranges and needn't reach their ends.
All inputs are finite; a program needn't handle non-finite values.
Results may differ from the reference program's by a relative error of at most 0.015.
The reference program's roundings to bfloat16 on the way count: a program that leaves them out, or rounds other values in their place, can miss the bound.
Values may be sent and summed in bfloat16 or wider, within the bound.
A program may use at most 128 MiB of HBM per device.

```python
import math
import jax
import jax.numpy as jnp
from jax import lax

D = 2048
HEADS = 8
HALF = 64
VDIM = 128
LENGTH = 2048
SEQS = 4
N_TP = 2


def gain_draw(key, salt):
    lowest = 0.8
    highest = 1.8
    fraction = jax.random.uniform(jax.random.fold_in(key, salt), (HALF,), jnp.float32)
    return jnp.exp(jnp.log(lowest) + fraction * (jnp.log(highest) - jnp.log(lowest)))


def draw_query_gain(key, part):
    return gain_draw(key, 31)


def draw_key_gain(key, part):
    return gain_draw(key, 57)


def steps_of(own_key, shape, pieces, least, largest):
    level, own = 1.0, jax.random.fold_in(own_key, 6)
    for dim, parts in pieces:
        draws = jnp.exp(jax.random.uniform(jax.random.fold_in(own, dim), (parts,), jnp.float32, least / len(pieces), largest / len(pieces)))
        level = level * jnp.repeat(draws, shape[dim] // parts).reshape([-1 if axis == dim else 1 for axis in range(len(shape))])
    return level


def centred(rng, extent, scale, most, cuts=(), kind=jnp.bfloat16):
    values = jax.random.normal(rng, extent, jnp.float32) * scale
    if len(cuts) > 0:
        values = steps_of(rng, extent, cuts, -0.22, 0.18) * values
    return jnp.clip(values, min=-most, max=most).astype(kind)


def setup_inputs(seed: int = 0) -> dict:
    keys = jax.random.split(jax.random.key(seed), 16)
    return {
        "inputs": centred(keys[0], (SEQS, LENGTH, D), 1.0, 6.0, ((0, 4), (1, 4), (2, 2))),
        "norm_gain": jnp.clip(1.0 + 0.18 * jax.random.normal(keys[1], (D,), jnp.float32), 0.1, 1.9),
        "query_weight": centred(keys[2], (D, HEADS * 2 * HALF), D ** -0.5, 0.125, ((0, 16), (1, 2))),
        "key_weight": centred(keys[3], (D, HEADS * 2 * HALF), D ** -0.5, 0.125, ((0, 16), (1, 2))),
        "value_weight": centred(keys[4], (D, HEADS * VDIM), D ** -0.5, 0.125, ((0, 16), (1, 2))),
        "query_gain": draw_query_gain(jax.random.fold_in(keys[15], 71), 0),
        "key_gain": draw_key_gain(jax.random.fold_in(keys[15], 71), 0),
        "mix_lambda": jnp.clip(jax.random.uniform(keys[7], (HEADS,), jnp.float32, 0.3, 0.8), 0.3, 0.8),
        "head_gain": jnp.clip(1.0 + 0.18 * jax.random.normal(keys[8], (VDIM,), jnp.float32), 0.1, 1.9),
        "post_gate_weight": centred(keys[9], (D, D), D ** -0.5, 0.125, ((0, 16), (1, 2))),
        "pre_gate_weight": centred(keys[10], (D, D), D ** -0.5, 0.125, ((0, 16), (1, 2))),
        "inner_weight": centred(keys[11], (D, D), D ** -0.5, 0.125, ((0, 16), (1, 2))),
        "conv_taps": centred(keys[12], (3, D), 0.6, 3.0, (), jnp.float32),
        "attn_out_weight": centred(keys[13], (D, HEADS * VDIM), (HEADS * VDIM + D) ** -0.5, 0.109375, ((0, 16), (1, 2))),
        "conv_out_weight": centred(keys[14], (D, D), (HEADS * VDIM + D) ** -0.5, 0.109375, ((0, 16), (1, 2))),
    }


epsilon = 1e-06

def scale_rows(values, gain):
    return values * lax.rsqrt(lax.optimization_barrier(jnp.mean(values * values, axis=-1, keepdims=True)) + epsilon) * gain

def attend_head(query_head, key_head, value_head, weight_two):
    block = math.gcd(LENGTH, 512)
    query_blocks = jnp.transpose(query_head.reshape(2, LENGTH // block, block, HALF), (1, 0, 2, 3))
    keys_wide = key_head.astype(jnp.float32)
    values_wide = value_head.astype(jnp.float32)

    def one_block(query_block):
        scores = jnp.einsum('jqd,jkd->jqk', query_block.astype(jnp.float32), keys_wide) * HALF ** (-0.5)
        peak = lax.optimization_barrier(jnp.max(scores, axis=-1, keepdims=True))
        expo = jnp.exp(scores - peak)
        total = lax.optimization_barrier(jnp.sum(expo, axis=-1, keepdims=True))
        rounded = lax.optimization_barrier(expo.astype(jnp.bfloat16)).astype(jnp.float32)
        mapped = jnp.einsum('jqk,kd->jqd', rounded, values_wide) / total
        return mapped[0] - weight_two * mapped[1]
    result = lax.map(one_block, query_blocks)
    return result.reshape(LENGTH, VDIM)

def one_sequence(tokens, norm_gain, query_weight, key_weight, value_weight, query_gain, key_gain, mix_lambda, head_gain, post_gate_weight, pre_gate_weight, inner_weight, conv_taps, attn_out_weight, conv_out_weight):
    normed = scale_rows(tokens.astype(jnp.float32), norm_gain).astype(jnp.bfloat16)
    query = jnp.dot(normed, query_weight, preferred_element_type=jnp.float32).reshape(LENGTH, HEADS, 2, HALF)
    key = jnp.dot(normed, key_weight, preferred_element_type=jnp.float32).reshape(LENGTH, HEADS, 2, HALF)
    query_normed = scale_rows(query, query_gain).astype(jnp.bfloat16)
    key_normed = scale_rows(key, key_gain).astype(jnp.bfloat16)
    values = jnp.dot(normed, value_weight, preferred_element_type=jnp.float32).astype(jnp.bfloat16)
    values = values.reshape(LENGTH, HEADS, VDIM)

    def per_head(members):
        return attend_head(members[0], members[1], members[2], members[3])
    head_out = lax.map(per_head, (jnp.transpose(query_normed, (1, 2, 0, 3)), jnp.transpose(key_normed, (1, 2, 0, 3)), jnp.transpose(values, (1, 0, 2)), mix_lambda))
    attn_hidden = scale_rows(head_out, head_gain).astype(jnp.bfloat16)
    attn_hidden = jnp.transpose(attn_hidden, (1, 0, 2)).reshape(LENGTH, HEADS * VDIM)
    post = jnp.dot(normed, post_gate_weight, preferred_element_type=jnp.float32).astype(jnp.bfloat16)
    post_wide = lax.optimization_barrier(post).astype(jnp.float32)
    signal = (jnp.dot(normed, pre_gate_weight, preferred_element_type=jnp.float32) * jnp.dot(normed, inner_weight, preferred_element_type=jnp.float32)).astype(jnp.bfloat16)
    padded = jnp.pad(lax.optimization_barrier(signal).astype(jnp.float32), ((1, 1), (0, 0)))
    filtered = conv_taps[0] * padded[:-2] + conv_taps[1] * padded[1:-1] + conv_taps[2] * padded[2:]
    conv_hidden = (post_wide * filtered).astype(jnp.bfloat16)
    head_span = HEADS // N_TP * VDIM
    channel_span = D // N_TP
    summed = jnp.zeros((LENGTH, D), jnp.float32)
    for group in range(N_TP):
        attn_part = attn_hidden[:, group * head_span:(group + 1) * head_span]
        attn_cols = attn_out_weight[:, group * head_span:(group + 1) * head_span]
        conv_part = conv_hidden[:, group * channel_span:(group + 1) * channel_span]
        conv_cols = conv_out_weight[:, group * channel_span:(group + 1) * channel_span]
        partial_value = jnp.dot(attn_part, attn_cols.T, preferred_element_type=jnp.float32) + jnp.dot(conv_part, conv_cols.T, preferred_element_type=jnp.float32)
        summed = summed + lax.optimization_barrier(partial_value.astype(jnp.bfloat16)).astype(jnp.float32)
    return summed.astype(jnp.bfloat16)

def reference(inputs, norm_gain, query_weight, key_weight, value_weight, query_gain, key_gain, mix_lambda, head_gain, post_gate_weight, pre_gate_weight, inner_weight, conv_taps, attn_out_weight, conv_out_weight):
    results = []
    for sequence in range(SEQS):
        results.append(one_sequence(inputs[sequence], norm_gain, query_weight, key_weight, value_weight, query_gain, key_gain, mix_lambda, head_gain, post_gate_weight, pre_gate_weight, inner_weight, conv_taps, attn_out_weight, conv_out_weight))
    return jnp.stack(results, axis=0)
```

```python
import math

import jax
import jax.numpy as jnp
from jax import lax
from jax.experimental import pallas as pl
from jax.experimental.pallas import tpu as pltpu
from jax.sharding import PartitionSpec as P

epsilon = 1e-06


def padded_2(x, sides, width):
    for axis, dim in sides:
        size, length = (lax.axis_size(axis), x.shape[dim])
        up = [(i, (i + 1) % size) for i in range(size - 1)]
        down = [(j, i) for i, j in up]
        last = lax.slice_in_dim(x, length - width, length, axis=dim)
        initial = lax.slice_in_dim(x, 0, width, axis=dim)
        before = lax.ppermute(last, axis, up)
        after = lax.ppermute(initial, axis, down)
        x = jnp.concatenate([before, x, after], axis=dim)
    return x


def scale_rows(values, gain):
    return values * lax.rsqrt(jnp.mean(values * values, axis=-1, keepdims=True) + epsilon) * gain


def project_all(normed, weights, products):
    result = []
    for member in range(len(weights)):
        if member < products:
            result.append(jnp.dot(normed, weights[member], preferred_element_type=jnp.float32))
        else:
            result.append(weights[member])
    return tuple(result)


def attention_branch(query, key, values, weight_two, query_gain, key_gain, head_gain):
    tok_rows = query.shape[0]
    vsize = head_gain.shape[0]
    half = query_gain.shape[0]
    heads = values.shape[1] // vsize
    query_normed = scale_rows(query.reshape(tok_rows, heads, 2, half), query_gain).astype(
        jnp.bfloat16
    )
    key_normed = scale_rows(key.reshape(tok_rows, heads * 2, half), key_gain).astype(jnp.bfloat16)
    key_normed = key_normed.reshape(tok_rows, heads * 2 * half)
    scale = half ** (-0.5)
    initial = (
        jnp.full((heads, 2, tok_rows), -1e30, jnp.float32),
        jnp.zeros((heads, 2, tok_rows), jnp.float32),
        jnp.zeros((heads, 2, tok_rows, vsize), jnp.float32),
    )
    carry = initial
    key_piece = lax.all_gather(key_normed, "sp", axis=0, tiled=True)
    value_piece = lax.all_gather(values, "sp", axis=0, tiled=True)
    length = key_piece.shape[0]
    block = math.gcd(length, 512)
    key_blocks = key_piece.reshape(length // block, block, heads, 2, half)
    value_blocks = value_piece.reshape(length // block, block, heads, vsize)

    def one_block(state, blocks):
        peak, total, accum = state
        key_block, value_block = blocks
        scores = (
            jnp.einsum(
                "qhjd,khjd->hjqk", query_normed, key_block, preferred_element_type=jnp.float32
            )
            * scale
        )
        new_peak = jnp.maximum(peak, jnp.max(scores, axis=-1))
        factor = jnp.exp(peak - new_peak)
        expo = jnp.exp(scores - new_peak[..., None])
        total = total * factor + jnp.sum(expo, axis=-1)
        accum = accum * factor[..., None] + jnp.einsum(
            "hjqk,khd->hjqd",
            expo.astype(jnp.bfloat16),
            value_block,
            preferred_element_type=jnp.float32,
        )
        return ((new_peak, total, accum), None)

    carry, unused = lax.scan(one_block, carry, (key_blocks, value_blocks))
    peak, total, accum = carry
    mapped = accum / total[..., None]
    head_out = mapped[:, 0] - weight_two[:, None, None] * mapped[:, 1]
    normed_out = scale_rows(head_out, head_gain).astype(jnp.bfloat16)
    return jnp.transpose(normed_out, (1, 0, 2)).reshape(tok_rows, heads * vsize)


def half_scaled(values, gain, half):
    low = lax.broadcasted_iota(jnp.int32, (1, 2 * half), 1) < half
    squares = values * values
    first = jnp.sum(jnp.where(low, squares, 0.0), axis=-1, keepdims=True) / half
    second = jnp.sum(jnp.where(low, 0.0, squares), axis=-1, keepdims=True) / half
    factor = jnp.where(low, lax.rsqrt(first + epsilon), lax.rsqrt(second + epsilon))
    return values * factor * gain


def attention_kernel(half, q_ref, k_ref, v_ref, qg_ref, kg_ref, lam_ref, hg_ref, out_ref, key, val):
    @pl.when(pl.program_id(1) == 0)
    def _():
        key[...] = half_scaled(k_ref[...], kg_ref[...], half).astype(jnp.bfloat16)
        val[...] = v_ref[...].astype(jnp.bfloat16)

    low = lax.broadcasted_iota(jnp.int32, (1, 2 * half), 1) < half
    query = half_scaled(q_ref[...], qg_ref[...], half).astype(jnp.bfloat16).astype(jnp.float32)
    maps = []
    for which in range(2):
        keep = low if which == 0 else jnp.logical_not(low)
        part = jnp.where(keep, query, 0.0).astype(jnp.bfloat16)
        scores = lax.dot_general(
            part, key[...], (((1,), (1,)), ((), ())), preferred_element_type=jnp.float32
        ) * half ** (-0.5)
        expo = jnp.exp(scores - jnp.max(scores, axis=-1, keepdims=True))
        total = jnp.sum(expo, axis=-1, keepdims=True)
        maps.append(
            jnp.dot(expo.astype(jnp.bfloat16), val[...], preferred_element_type=jnp.float32) / total
        )
    head_out = maps[0] - lam_ref[0] * maps[1]
    out_ref[...] = scale_rows(head_out, hg_ref[...]).astype(jnp.bfloat16)


def attention_call(y, heads, query_gain, key_gain, weight_two, head_gain):
    rows = y.shape[0]
    half, vsize = query_gain.shape[0], head_gain.shape[0]
    block = math.gcd(rows, 256)
    small = lambda h, i: (0, 0)
    return pl.pallas_call(
        lambda *refs: attention_kernel(half, *refs),
        out_shape=jax.ShapeDtypeStruct((rows, heads * vsize), jnp.bfloat16),
        grid=(heads, rows // block),
        in_specs=[
            pl.BlockSpec((block, 2 * half), lambda h, i: (i, h)),
            pl.BlockSpec((rows, 2 * half), lambda h, i: (0, heads + h)),
            pl.BlockSpec((rows, vsize), lambda h, i: (0, 2 * heads + h)),
            pl.BlockSpec((1, 2 * half), small),
            pl.BlockSpec((1, 2 * half), small),
            pl.BlockSpec((1, 1, vsize), lambda h, i: (h, 0, 0)),
            pl.BlockSpec((1, vsize), small),
        ],
        out_specs=pl.BlockSpec((block, vsize), lambda h, i: (i, h)),
        scratch_shapes=[
            pltpu.VMEM((rows, 2 * half), jnp.bfloat16),
            pltpu.VMEM((rows, vsize), jnp.bfloat16),
        ],
        compiler_params=pltpu.CompilerParams(vmem_limit_bytes=40 * 2**20),
        cost_estimate=pl.CostEstimate(
            flops=heads * rows * rows * 8 * half * 2,
            bytes_accessed=rows * heads * vsize * 14,
            transcendentals=2 * heads * rows * rows,
        ),
    )(
        y,
        y,
        y,
        jnp.tile(query_gain, 2)[None],
        jnp.tile(key_gain, 2)[None],
        jnp.broadcast_to(weight_two[:, None, None], (heads, 1, vsize)),
        head_gain[None],
    )


def column_parts(weights, parts):
    rows = weights[0].shape[0]
    pieces = [w.reshape(rows, parts, w.shape[1] // parts) for w in weights]
    return jnp.transpose(jnp.concatenate(pieces, axis=2), (1, 0, 2))


def gathered_rows(packed):
    mine = lax.all_to_all(packed, "sp", split_axis=0, concat_axis=0, tiled=True)
    every = lax.all_gather(mine, "fs", axis=1, tiled=False)
    return every.reshape(-1, packed.shape[2])


def split_device(
    inputs,
    norm_gain,
    query_weight,
    key_weight,
    value_weight,
    query_gain,
    key_gain,
    mix_lambda,
    head_gain,
    post_gate_weight,
    pre_gate_weight,
    inner_weight,
    conv_taps,
    attn_out_weight,
    conv_out_weight,
):
    sp, tp = lax.axis_size("sp"), lax.axis_size("tp")
    tokens = inputs[0]
    place = lax.axis_index("tp") * sp + lax.axis_index("sp")
    vsize = head_gain.shape[0]
    heads = value_weight.shape[1] // vsize // sp
    channels = post_gate_weight.shape[1] // sp
    weight_two = lax.dynamic_slice_in_dim(mix_lambda, place * heads, heads)
    taps = lax.dynamic_slice_in_dim(conv_taps, place * channels, channels, 1)
    into = gathered_rows(
        column_parts(
            (query_weight, key_weight, value_weight, post_gate_weight, pre_gate_weight, inner_weight),
            sp,
        )
    )
    outof = gathered_rows(column_parts((attn_out_weight, conv_out_weight), sp))
    along = lax.all_gather(tokens, "sp", axis=0, tiled=True)
    both = lax.all_gather(along, "tp", axis=0, tiled=False)
    whole = jnp.concatenate([both[i] for i in range(tp)], axis=1)
    normed = scale_rows(whole.astype(jnp.float32), norm_gain).astype(jnp.bfloat16)
    y = jnp.dot(normed, into, preferred_element_type=jnp.float32)
    attn_hidden = attention_call(y, heads, query_gain, key_gain, weight_two, head_gain)
    span = 3 * heads * vsize
    post, pre_gate, inner = [
        y[:, span + i * channels : span + (i + 1) * channels] for i in range(3)
    ]
    post_wide = lax.optimization_barrier(post.astype(jnp.bfloat16)).astype(jnp.float32)
    signal = lax.optimization_barrier((pre_gate * inner).astype(jnp.bfloat16))
    shifted = jnp.pad(signal.astype(jnp.float32), ((1, 1), (0, 0)))
    filtered = taps[0] * shifted[:-2] + taps[1] * shifted[1:-1] + taps[2] * shifted[2:]
    conv_hidden = (post_wide * filtered).astype(jnp.bfloat16)
    hidden = jnp.concatenate([attn_hidden, conv_hidden], axis=1)
    width = hidden.shape[1]
    hidden = hidden.reshape(sp, tp, -1, width).transpose(1, 0, 2, 3).reshape(-1, width)
    partial = lax.dot_general(
        hidden, outof, (((1,), (1,)), ((), ())), preferred_element_type=jnp.float32
    ).astype(jnp.bfloat16)
    summed = lax.psum_scatter(partial, "tp", scatter_dimension=0, tiled=True)
    summed = lax.psum_scatter(summed, "sp", scatter_dimension=0, tiled=True)
    return summed[None]


def per_device(
    inputs,
    norm_gain,
    query_weight,
    key_weight,
    value_weight,
    query_gain,
    key_gain,
    mix_lambda,
    head_gain,
    post_gate_weight,
    pre_gate_weight,
    inner_weight,
    conv_taps,
    attn_out_weight,
    conv_out_weight,
):
    tokens = inputs[0]
    whole = lax.all_gather(tokens, "tp", axis=1, tiled=True)
    normed = scale_rows(whole.astype(jnp.float32), norm_gain).astype(jnp.bfloat16)
    heads_dev = value_weight.shape[1] // head_gain.shape[0]
    channels = post_gate_weight.shape[1]
    tp_index = lax.axis_index("tp")
    weight_two = lax.dynamic_slice_in_dim(mix_lambda, tp_index * heads_dev, heads_dev)
    taps = lax.dynamic_slice_in_dim(conv_taps, tp_index * channels, channels, 1)
    every_full = (
        lax.all_gather(query_weight, ("sp", "fs"), axis=0, tiled=True),
        lax.all_gather(key_weight, ("sp", "fs"), axis=0, tiled=True),
        lax.all_gather(value_weight, ("sp", "fs"), axis=0, tiled=True),
        lax.all_gather(post_gate_weight, ("sp", "fs"), axis=0, tiled=True),
        lax.all_gather(pre_gate_weight, ("sp", "fs"), axis=0, tiled=True),
        lax.all_gather(inner_weight, ("sp", "fs"), axis=0, tiled=True),
        lax.all_gather(attn_out_weight, ("sp", "fs"), axis=0, tiled=True),
        lax.all_gather(conv_out_weight, ("sp", "fs"), axis=0, tiled=True),
    )
    query, key, value_proj, post, pre_gate, inner, attn_out_full, conv_out_full = project_all(
        normed, every_full[0:3] + every_full[3:6] + every_full[6:8], 6
    )
    attn_hidden = attention_branch(
        query, key, value_proj.astype(jnp.bfloat16), weight_two, query_gain, key_gain, head_gain
    )
    post_mid = post.astype(jnp.bfloat16)
    post_wide = lax.optimization_barrier(post_mid).astype(jnp.float32)
    signal = (pre_gate * inner).astype(jnp.bfloat16)
    padded = padded_2(signal, (("sp", 0),), 1)
    shifted = lax.optimization_barrier(padded).astype(jnp.float32)
    filtered = taps[0] * shifted[:-2] + taps[1] * shifted[1:-1] + taps[2] * shifted[2:]
    conv_hidden = (post_wide * filtered).astype(jnp.bfloat16)
    contract = (((1,), (1,)), ((), ()))
    summed = lax.psum_scatter(
        (
            lax.dot_general(
                attn_hidden, attn_out_full, contract, preferred_element_type=jnp.float32
            )
            + lax.dot_general(
                conv_hidden, conv_out_full, contract, preferred_element_type=jnp.float32
            )
        ).astype(jnp.bfloat16),
        "tp",
        scatter_dimension=0,
        tiled=True,
    )
    return summed[None]


def solution(mesh):
    placed = (
        P("fs", "sp", "tp"),
        P(),
        P(("sp", "fs"), "tp"),
        P(("sp", "fs"), "tp"),
        P(("sp", "fs"), "tp"),
        P(),
        P(),
        P(),
        P(),
        P(("sp", "fs"), "tp"),
        P(("sp", "fs"), "tp"),
        P(("sp", "fs"), "tp"),
        P(),
        P(("sp", "fs"), "tp"),
        P(("sp", "fs"), "tp"),
    )
    sp, tp = mesh.shape["sp"], mesh.shape["tp"]

    def program(*args):
        heads = args[7].shape[0]
        channels = args[12].shape[1]
        splits = heads % (sp * tp) == 0 and channels % (sp * tp * 128) == 0
        return shard(split_device if splits else per_device)(*args)

    shard = lambda body: jax.shard_map(
        body,
        mesh=mesh,
        in_specs=placed,
        out_specs=P("fs", ("sp", "tp"), None),
        check_vma=False,
    )

    return program
```

```python
import math

import jax
import jax.numpy as jnp
from jax import lax
from jax.experimental import pallas as pl
from jax.experimental.pallas import tpu as pltpu
from jax.sharding import PartitionSpec as P

epsilon = 1e-06


def padded_2(x, sides, width):
    for axis, dim in sides:
        size, length = (lax.axis_size(axis), x.shape[dim])
        up = [(i, (i + 1) % size) for i in range(size - 1)]
        down = [(j, i) for i, j in up]
        last = lax.slice_in_dim(x, length - width, length, axis=dim)
        initial = lax.slice_in_dim(x, 0, width, axis=dim)
        before = lax.ppermute(last, axis, up)
        after = lax.ppermute(initial, axis, down)
        x = jnp.concatenate([before, x, after], axis=dim)
    return x


def scale_rows(values, gain):
    return values * lax.rsqrt(jnp.mean(values * values, axis=-1, keepdims=True) + epsilon) * gain


def project_all(normed, weights, products):
    result = []
    for member in range(len(weights)):
        if member < products:
            result.append(jnp.dot(normed, weights[member], preferred_element_type=jnp.float32))
        else:
            result.append(weights[member])
    return tuple(result)


def attention_branch(query, key, values, weight_two, query_gain, key_gain, head_gain):
    tok_rows = query.shape[0]
    vsize = head_gain.shape[0]
    half = query_gain.shape[0]
    heads = values.shape[1] // vsize
    query_normed = scale_rows(query.reshape(tok_rows, heads, 2, half), query_gain).astype(
        jnp.bfloat16
    )
    key_normed = scale_rows(key.reshape(tok_rows, heads * 2, half), key_gain).astype(jnp.bfloat16)
    key_normed = key_normed.reshape(tok_rows, heads * 2 * half)
    scale = half ** (-0.5)
    initial = (
        jnp.full((heads, 2, tok_rows), -1e30, jnp.float32),
        jnp.zeros((heads, 2, tok_rows), jnp.float32),
        jnp.zeros((heads, 2, tok_rows, vsize), jnp.float32),
    )
    carry = initial
    key_piece = lax.all_gather(key_normed, "sp", axis=0, tiled=True)
    value_piece = lax.all_gather(values, "sp", axis=0, tiled=True)
    length = key_piece.shape[0]
    block = math.gcd(length, 512)
    key_blocks = key_piece.reshape(length // block, block, heads, 2, half)
    value_blocks = value_piece.reshape(length // block, block, heads, vsize)

    def one_block(state, blocks):
        peak, total, accum = state
        key_block, value_block = blocks
        scores = (
            jnp.einsum(
                "qhjd,khjd->hjqk", query_normed, key_block, preferred_element_type=jnp.float32
            )
            * scale
        )
        new_peak = jnp.maximum(peak, jnp.max(scores, axis=-1))
        factor = jnp.exp(peak - new_peak)
        expo = jnp.exp(scores - new_peak[..., None])
        total = total * factor + jnp.sum(expo, axis=-1)
        accum = accum * factor[..., None] + jnp.einsum(
            "hjqk,khd->hjqd",
            expo.astype(jnp.bfloat16),
            value_block,
            preferred_element_type=jnp.float32,
        )
        return ((new_peak, total, accum), None)

    carry, unused = lax.scan(one_block, carry, (key_blocks, value_blocks))
    peak, total, accum = carry
    mapped = accum / total[..., None]
    head_out = mapped[:, 0] - weight_two[:, None, None] * mapped[:, 1]
    normed_out = scale_rows(head_out, head_gain).astype(jnp.bfloat16)
    return jnp.transpose(normed_out, (1, 0, 2)).reshape(tok_rows, heads * vsize)


def half_scaled(values, gain, half):
    low = lax.broadcasted_iota(jnp.int32, (1, 2 * half), 1) < half
    squares = values * values
    first = jnp.sum(jnp.where(low, squares, 0.0), axis=-1, keepdims=True) / half
    second = jnp.sum(jnp.where(low, 0.0, squares), axis=-1, keepdims=True) / half
    factor = jnp.where(low, lax.rsqrt(first + epsilon), lax.rsqrt(second + epsilon))
    return values * factor * gain


def attention_kernel(half, q_ref, k_ref, v_ref, qg_ref, kg_ref, lam_ref, hg_ref, out_ref, key, val):
    @pl.when(pl.program_id(1) == 0)
    def _():
        key[...] = half_scaled(k_ref[...], kg_ref[...], half).astype(jnp.bfloat16)
        val[...] = v_ref[...].astype(jnp.bfloat16)

    low = lax.broadcasted_iota(jnp.int32, (1, 2 * half), 1) < half
    query = half_scaled(q_ref[...], qg_ref[...], half).astype(jnp.bfloat16).astype(jnp.float32)
    maps = []
    for which in range(2):
        keep = low if which == 0 else jnp.logical_not(low)
        part = jnp.where(keep, query, 0.0).astype(jnp.bfloat16)
        scores = lax.dot_general(
            part, key[...], (((1,), (1,)), ((), ())), preferred_element_type=jnp.float32
        ) * half ** (-0.5)
        expo = jnp.exp(scores - jnp.max(scores, axis=-1, keepdims=True))
        total = jnp.sum(expo, axis=-1, keepdims=True)
        maps.append(
            jnp.dot(expo.astype(jnp.bfloat16), val[...], preferred_element_type=jnp.float32) / total
        )
    head_out = maps[0] - lam_ref[0] * maps[1]
    out_ref[...] = scale_rows(head_out, hg_ref[...]).astype(jnp.bfloat16)


def attention_call(y, heads, query_gain, key_gain, weight_two, head_gain):
    rows = y.shape[0]
    half, vsize = query_gain.shape[0], head_gain.shape[0]
    block = math.gcd(rows, 256)
    small = lambda h, i: (0, 0)
    return pl.pallas_call(
        lambda *refs: attention_kernel(half, *refs),
        out_shape=jax.ShapeDtypeStruct((rows, heads * vsize), jnp.bfloat16),
        grid=(heads, rows // block),
        in_specs=[
            pl.BlockSpec((block, 2 * half), lambda h, i: (i, h)),
            pl.BlockSpec((rows, 2 * half), lambda h, i: (0, heads + h)),
            pl.BlockSpec((rows, vsize), lambda h, i: (0, 2 * heads + h)),
            pl.BlockSpec((1, 2 * half), small),
            pl.BlockSpec((1, 2 * half), small),
            pl.BlockSpec((1, 1, vsize), lambda h, i: (h, 0, 0)),
            pl.BlockSpec((1, vsize), small),
        ],
        out_specs=pl.BlockSpec((block, vsize), lambda h, i: (i, h)),
        scratch_shapes=[
            pltpu.VMEM((rows, 2 * half), jnp.bfloat16),
            pltpu.VMEM((rows, vsize), jnp.bfloat16),
        ],
        compiler_params=pltpu.CompilerParams(vmem_limit_bytes=40 * 2**20),
        cost_estimate=pl.CostEstimate(
            flops=heads * rows * rows * 8 * half * 2,
            bytes_accessed=rows * heads * vsize * 14,
            transcendentals=2 * heads * rows * rows,
        ),
    )(
        y,
        y,
        y,
        jnp.tile(query_gain, 2)[None],
        jnp.tile(key_gain, 2)[None],
        jnp.broadcast_to(weight_two[:, None, None], (heads, 1, vsize)),
        head_gain[None],
    )


def column_parts(weights, parts):
    rows = weights[0].shape[0]
    pieces = [w.reshape(rows, parts, w.shape[1] // parts) for w in weights]
    return jnp.transpose(jnp.concatenate(pieces, axis=2), (1, 0, 2))


def remote(source, target, send, recv, where):
    return pltpu.make_async_remote_copy(
        src_ref=source,
        dst_ref=target,
        send_sem=send,
        recv_sem=recv,
        device_id=where,
        device_id_type=pl.DeviceIdType.MESH,
    )


def meet(places):
    barrier = pltpu.get_barrier_semaphore()
    for where in places:
        pl.semaphore_signal(
            barrier, inc=1, device_id=where, device_id_type=pl.DeviceIdType.MESH
        )
    pl.semaphore_wait(barrier, len(places))


def gather_kernel(
    n, w_ref, t_ref, w_all, t_all, own, z_send, z_recv, f_send, f_recv, g_send, g_recv,
    t_send, t_recv, p_send, p_recv,
):
    z, f, c = lax.axis_index("sp"), lax.axis_index("fs"), lax.axis_index("tp")
    beside, above = f + 1 - 2 * (f % 2), f + 2 - 4 * (f // 2)
    rows = t_ref.shape[0]
    near = sorted(range(1, n), key=lambda d: min(d, n - d))
    meet(
        [{"sp": (z + d) % n} for d in near] + [{"fs": beside}, {"fs": above}, {"tp": 1 - c}]
    )

    def place(s):
        return t_all.at[c, pl.ds(pl.multiple_of(s * rows, rows), rows)]

    flights = []

    def go(copy):
        copy.start()
        flights.append(copy)
        return copy

    across = {
        d: go(
            remote(
                w_ref.at[(z + d) % n], w_all.at[z, f], z_send.at[d], z_recv.at[d], {"sp": (z + d) % n}
            )
        )
        for d in near
    }
    side = {}

    def spread(d, source):
        s = (z + n - d) % n
        for i, to in enumerate((beside, above)):
            side[i, d] = go(
                remote(source, w_all.at[s, f], f_send.at[i, d], f_recv.at[i, d], {"fs": to})
            )

    def pass_on(d):
        s = (z + n - d) % n
        i = d % 2
        side[i, d].wait_recv()
        held, to = (beside, above) if i == 0 else (above, beside)
        go(remote(w_all.at[s, held], w_all.at[s, held], g_send.at[d], g_recv.at[d], {"fs": to}))

    spread(0, w_ref.at[z])
    tokens = {
        d: go(remote(t_ref, place(z), t_send.at[d], t_recv.at[d], {"sp": (z + d) % n}))
        for d in near
    }
    go(remote(t_ref, place(z), p_send.at[0], p_recv.at[0], {"tp": 1 - c}))
    mine = [
        pltpu.make_async_copy(w_ref.at[z], w_all.at[z, f], own.at[0]),
        pltpu.make_async_copy(t_ref, place(z), own.at[1]),
    ]
    for copy in mine:
        copy.start()
    last = 0
    for d in near:
        across[d].wait_recv()
        spread(d, w_all.at[(z + n - d) % n, f])
        pass_on(last)
        last = d
    pass_on(last)
    for d in near:
        tokens[d].wait_recv()
        s = (z + n - d) % n
        go(remote(place(s), place(s), p_send.at[d], p_recv.at[d], {"tp": 1 - c}))
    waited = set(map(id, across.values())) | set(map(id, tokens.values()))
    waited |= {id(side[d % 2, d]) for d in range(n)}
    for copy in flights:
        copy.wait_send()
        if id(copy) not in waited:
            copy.wait_recv()
    for copy in mine:
        copy.wait()


def gather_all(packed, tokens):
    n, rows, columns = packed.shape
    fs, tp = lax.axis_size("fs"), lax.axis_size("tp")
    dma = pltpu.SemaphoreType.DMA
    return pl.pallas_call(
        lambda *refs: gather_kernel(n, *refs),
        out_shape=(
            jax.ShapeDtypeStruct((n, fs, rows, columns), packed.dtype),
            jax.ShapeDtypeStruct((tp, n * tokens.shape[0], tokens.shape[1]), tokens.dtype),
        ),
        in_specs=[pl.BlockSpec(memory_space=pltpu.VMEM)] * 2,
        out_specs=(pl.BlockSpec(memory_space=pl.ANY),) * 2,
        scratch_shapes=[
            dma((2,)), dma((n,)), dma((n,)), dma((2, n)), dma((2, n)), dma((n,)), dma((n,)),
            dma((n,)), dma((n,)), dma((n,)), dma((n,)),
        ],
        compiler_params=pltpu.CompilerParams(collective_id=1, has_side_effects=True),
    )(packed, tokens)


def reduce_kernel(n, p_ref, out_ref, twin, pair, others, a_send, a_recv, b_send, b_recv):
    z, c = lax.axis_index("sp"), lax.axis_index("tp")
    near = sorted(range(1, n), key=lambda d: -min(d, n - d))
    meet([{"sp": (z + d) % n} for d in near] + [{"tp": 1 - c}])
    rows = out_ref.shape[0]
    tile = math.gcd(rows, 32)
    swaps = {}
    for d in near + [0]:
        s = (z + d) % n
        swaps[d] = remote(
            p_ref.at[1 - c, s], twin.at[d], a_send.at[d], a_recv.at[d], {"tp": 1 - c}
        )
        swaps[d].start()
    sends = {}
    for d in near + [0]:
        s = (z + d) % n
        swaps[d].wait_recv()

        def add(i, unused, s=s, d=d):
            at = pl.ds(pl.multiple_of(i * tile, tile), tile)
            total = p_ref[c, s, at, :].astype(jnp.float32) + twin[d, at, :].astype(jnp.float32)
            pair[d, at, :] = total.astype(jnp.bfloat16)
            return unused

        lax.fori_loop(0, rows // tile, add, 0)
        if d:
            sends[d] = remote(
                pair.at[d], others.at[d - 1], b_send.at[d - 1], b_recv.at[d - 1], {"sp": s}
            )
            sends[d].start()
    for d in near:
        sends[d].wait_recv()

    def finish(i, unused):
        at = pl.ds(pl.multiple_of(i * tile, tile), tile)
        total = pair[0, at, :].astype(jnp.float32)
        for d in range(1, n):
            total += others[d - 1, at, :].astype(jnp.float32)
        out_ref[at, :] = total.astype(jnp.bfloat16)
        return unused

    lax.fori_loop(0, rows // tile, finish, 0)
    for d in near + [0]:
        swaps[d].wait_send()
    for d in near:
        sends[d].wait_send()


def reduce_all(partial):
    tp, n, rows, width = partial.shape
    dma = pltpu.SemaphoreType.DMA
    return pl.pallas_call(
        lambda *refs: reduce_kernel(n, *refs),
        out_shape=jax.ShapeDtypeStruct((rows, width), partial.dtype),
        in_specs=[pl.BlockSpec(memory_space=pltpu.VMEM)],
        out_specs=pl.BlockSpec(memory_space=pltpu.VMEM),
        scratch_shapes=[
            pltpu.VMEM((n, rows, width), partial.dtype),
            pltpu.VMEM((n, rows, width), partial.dtype),
            pltpu.VMEM((n - 1, rows, width), partial.dtype),
            dma((n,)), dma((n,)), dma((n - 1,)), dma((n - 1,)),
        ],
        compiler_params=pltpu.CompilerParams(
            collective_id=2, has_side_effects=True, vmem_limit_bytes=48 * 2**20
        ),
    )(partial)


def split_device(
    inputs,
    norm_gain,
    query_weight,
    key_weight,
    value_weight,
    query_gain,
    key_gain,
    mix_lambda,
    head_gain,
    post_gate_weight,
    pre_gate_weight,
    inner_weight,
    conv_taps,
    attn_out_weight,
    conv_out_weight,
):
    sp, tp = lax.axis_size("sp"), lax.axis_size("tp")
    tokens = inputs[0]
    place = lax.axis_index("tp") * sp + lax.axis_index("sp")
    vsize = head_gain.shape[0]
    heads = value_weight.shape[1] // vsize // sp
    channels = post_gate_weight.shape[1] // sp
    weight_two = lax.dynamic_slice_in_dim(mix_lambda, place * heads, heads)
    taps = lax.dynamic_slice_in_dim(conv_taps, place * channels, channels, 1)
    packed = column_parts(
        (
            query_weight,
            key_weight,
            value_weight,
            post_gate_weight,
            pre_gate_weight,
            inner_weight,
            attn_out_weight,
            conv_out_weight,
        ),
        sp,
    )
    every, both = gather_all(packed, tokens)
    every = every.reshape(-1, packed.shape[2])
    cut = 3 * heads * vsize + 3 * channels
    into, outof = every[:, :cut], every[:, cut:]
    whole = jnp.concatenate([both[i] for i in range(tp)], axis=1)
    normed = scale_rows(whole.astype(jnp.float32), norm_gain).astype(jnp.bfloat16)
    y = jnp.dot(normed, into, preferred_element_type=jnp.float32)
    attn_hidden = attention_call(y, heads, query_gain, key_gain, weight_two, head_gain)
    span = 3 * heads * vsize
    post, pre_gate, inner = [
        y[:, span + i * channels : span + (i + 1) * channels] for i in range(3)
    ]
    post_wide = lax.optimization_barrier(post.astype(jnp.bfloat16)).astype(jnp.float32)
    signal = lax.optimization_barrier((pre_gate * inner).astype(jnp.bfloat16))
    shifted = jnp.pad(signal.astype(jnp.float32), ((1, 1), (0, 0)))
    filtered = taps[0] * shifted[:-2] + taps[1] * shifted[1:-1] + taps[2] * shifted[2:]
    conv_hidden = (post_wide * filtered).astype(jnp.bfloat16)
    hidden = jnp.concatenate([attn_hidden, conv_hidden], axis=1)
    width = hidden.shape[1]
    hidden = hidden.reshape(sp, tp, -1, width).transpose(1, 0, 2, 3).reshape(-1, width)
    partial = lax.dot_general(
        hidden, outof, (((1,), (1,)), ((), ())), preferred_element_type=jnp.float32
    ).astype(jnp.bfloat16)
    summed = reduce_all(partial.reshape(tp, sp, -1, partial.shape[1]))
    return summed[None]


def per_device(
    inputs,
    norm_gain,
    query_weight,
    key_weight,
    value_weight,
    query_gain,
    key_gain,
    mix_lambda,
    head_gain,
    post_gate_weight,
    pre_gate_weight,
    inner_weight,
    conv_taps,
    attn_out_weight,
    conv_out_weight,
):
    tokens = inputs[0]
    whole = lax.all_gather(tokens, "tp", axis=1, tiled=True)
    normed = scale_rows(whole.astype(jnp.float32), norm_gain).astype(jnp.bfloat16)
    heads_dev = value_weight.shape[1] // head_gain.shape[0]
    channels = post_gate_weight.shape[1]
    tp_index = lax.axis_index("tp")
    weight_two = lax.dynamic_slice_in_dim(mix_lambda, tp_index * heads_dev, heads_dev)
    taps = lax.dynamic_slice_in_dim(conv_taps, tp_index * channels, channels, 1)
    every_full = (
        lax.all_gather(query_weight, ("sp", "fs"), axis=0, tiled=True),
        lax.all_gather(key_weight, ("sp", "fs"), axis=0, tiled=True),
        lax.all_gather(value_weight, ("sp", "fs"), axis=0, tiled=True),
        lax.all_gather(post_gate_weight, ("sp", "fs"), axis=0, tiled=True),
        lax.all_gather(pre_gate_weight, ("sp", "fs"), axis=0, tiled=True),
        lax.all_gather(inner_weight, ("sp", "fs"), axis=0, tiled=True),
        lax.all_gather(attn_out_weight, ("sp", "fs"), axis=0, tiled=True),
        lax.all_gather(conv_out_weight, ("sp", "fs"), axis=0, tiled=True),
    )
    query, key, value_proj, post, pre_gate, inner, attn_out_full, conv_out_full = project_all(
        normed, every_full[0:3] + every_full[3:6] + every_full[6:8], 6
    )
    attn_hidden = attention_branch(
        query, key, value_proj.astype(jnp.bfloat16), weight_two, query_gain, key_gain, head_gain
    )
    post_mid = post.astype(jnp.bfloat16)
    post_wide = lax.optimization_barrier(post_mid).astype(jnp.float32)
    signal = (pre_gate * inner).astype(jnp.bfloat16)
    padded = padded_2(signal, (("sp", 0),), 1)
    shifted = lax.optimization_barrier(padded).astype(jnp.float32)
    filtered = taps[0] * shifted[:-2] + taps[1] * shifted[1:-1] + taps[2] * shifted[2:]
    conv_hidden = (post_wide * filtered).astype(jnp.bfloat16)
    contract = (((1,), (1,)), ((), ()))
    summed = lax.psum_scatter(
        (
            lax.dot_general(
                attn_hidden, attn_out_full, contract, preferred_element_type=jnp.float32
            )
            + lax.dot_general(
                conv_hidden, conv_out_full, contract, preferred_element_type=jnp.float32
            )
        ).astype(jnp.bfloat16),
        "tp",
        scatter_dimension=0,
        tiled=True,
    )
    return summed[None]


def solution(mesh):
    placed = (
        P("fs", "sp", "tp"),
        P(),
        P(("sp", "fs"), "tp"),
        P(("sp", "fs"), "tp"),
        P(("sp", "fs"), "tp"),
        P(),
        P(),
        P(),
        P(),
        P(("sp", "fs"), "tp"),
        P(("sp", "fs"), "tp"),
        P(("sp", "fs"), "tp"),
        P(),
        P(("sp", "fs"), "tp"),
        P(("sp", "fs"), "tp"),
    )
    sp, tp = mesh.shape["sp"], mesh.shape["tp"]

    def program(*args):
        heads = args[7].shape[0]
        channels = args[12].shape[1]
        splits = tp == 2 and mesh.shape["fs"] == 4 and sp > 1 and heads % (sp * tp) == 0
        splits = splits and channels % (sp * tp * 128) == 0
        return shard(split_device if splits else per_device)(*args)

    shard = lambda body: jax.shard_map(
        body,
        mesh=mesh,
        in_specs=placed,
        out_specs=P("fs", ("sp", "tp"), None),
        check_vma=False,
    )

    return program
```

```python
import math

import jax
import jax.numpy as jnp
from jax import lax
from jax.experimental import pallas as pl
from jax.experimental.pallas import tpu as pltpu
from jax.sharding import PartitionSpec as P

epsilon = 1e-06


def padded_2(x, sides, width):
    for axis, dim in sides:
        size, length = (lax.axis_size(axis), x.shape[dim])
        up = [(i, (i + 1) % size) for i in range(size - 1)]
        down = [(j, i) for i, j in up]
        last = lax.slice_in_dim(x, length - width, length, axis=dim)
        initial = lax.slice_in_dim(x, 0, width, axis=dim)
        before = lax.ppermute(last, axis, up)
        after = lax.ppermute(initial, axis, down)
        x = jnp.concatenate([before, x, after], axis=dim)
    return x


def scale_rows(values, gain):
    return values * lax.rsqrt(jnp.mean(values * values, axis=-1, keepdims=True) + epsilon) * gain


def project_all(normed, weights, products):
    result = []
    for member in range(len(weights)):
        if member < products:
            result.append(jnp.dot(normed, weights[member], preferred_element_type=jnp.float32))
        else:
            result.append(weights[member])
    return tuple(result)


def attention_branch(query, key, values, weight_two, query_gain, key_gain, head_gain):
    tok_rows = query.shape[0]
    vsize = head_gain.shape[0]
    half = query_gain.shape[0]
    heads = values.shape[1] // vsize
    query_normed = scale_rows(query.reshape(tok_rows, heads, 2, half), query_gain).astype(
        jnp.bfloat16
    )
    key_normed = scale_rows(key.reshape(tok_rows, heads * 2, half), key_gain).astype(jnp.bfloat16)
    key_normed = key_normed.reshape(tok_rows, heads * 2 * half)
    scale = half ** (-0.5)
    initial = (
        jnp.full((heads, 2, tok_rows), -1e30, jnp.float32),
        jnp.zeros((heads, 2, tok_rows), jnp.float32),
        jnp.zeros((heads, 2, tok_rows, vsize), jnp.float32),
    )
    carry = initial
    key_piece = lax.all_gather(key_normed, "sp", axis=0, tiled=True)
    value_piece = lax.all_gather(values, "sp", axis=0, tiled=True)
    length = key_piece.shape[0]
    block = math.gcd(length, 512)
    key_blocks = key_piece.reshape(length // block, block, heads, 2, half)
    value_blocks = value_piece.reshape(length // block, block, heads, vsize)

    def one_block(state, blocks):
        peak, total, accum = state
        key_block, value_block = blocks
        scores = (
            jnp.einsum(
                "qhjd,khjd->hjqk", query_normed, key_block, preferred_element_type=jnp.float32
            )
            * scale
        )
        new_peak = jnp.maximum(peak, jnp.max(scores, axis=-1))
        factor = jnp.exp(peak - new_peak)
        expo = jnp.exp(scores - new_peak[..., None])
        total = total * factor + jnp.sum(expo, axis=-1)
        accum = accum * factor[..., None] + jnp.einsum(
            "hjqk,khd->hjqd",
            expo.astype(jnp.bfloat16),
            value_block,
            preferred_element_type=jnp.float32,
        )
        return ((new_peak, total, accum), None)

    carry, unused = lax.scan(one_block, carry, (key_blocks, value_blocks))
    peak, total, accum = carry
    mapped = accum / total[..., None]
    head_out = mapped[:, 0] - weight_two[:, None, None] * mapped[:, 1]
    normed_out = scale_rows(head_out, head_gain).astype(jnp.bfloat16)
    return jnp.transpose(normed_out, (1, 0, 2)).reshape(tok_rows, heads * vsize)


def half_scaled(values, gain, half):
    low = lax.broadcasted_iota(jnp.int32, (1, 2 * half), 1) < half
    squares = values * values
    first = jnp.sum(jnp.where(low, squares, 0.0), axis=-1, keepdims=True) / half
    second = jnp.sum(jnp.where(low, 0.0, squares), axis=-1, keepdims=True) / half
    factor = jnp.where(low, lax.rsqrt(first + epsilon), lax.rsqrt(second + epsilon))
    return values * factor * gain


def attention_kernel(half, q_ref, k_ref, v_ref, qg_ref, kg_ref, lam_ref, hg_ref, out_ref, key, val):
    @pl.when(pl.program_id(1) == 0)
    def _():
        key[...] = half_scaled(k_ref[...], kg_ref[...], half).astype(jnp.bfloat16)
        val[...] = v_ref[...].astype(jnp.bfloat16)

    low = lax.broadcasted_iota(jnp.int32, (1, 2 * half), 1) < half
    query = half_scaled(q_ref[...], qg_ref[...], half).astype(jnp.bfloat16).astype(jnp.float32)
    maps = []
    for which in range(2):
        keep = low if which == 0 else jnp.logical_not(low)
        part = jnp.where(keep, query, 0.0).astype(jnp.bfloat16)
        scores = lax.dot_general(
            part, key[...], (((1,), (1,)), ((), ())), preferred_element_type=jnp.float32
        ) * half ** (-0.5)
        expo = jnp.exp(scores - jnp.max(scores, axis=-1, keepdims=True))
        total = jnp.sum(expo, axis=-1, keepdims=True)
        maps.append(
            jnp.dot(expo.astype(jnp.bfloat16), val[...], preferred_element_type=jnp.float32) / total
        )
    head_out = maps[0] - lam_ref[0] * maps[1]
    out_ref[...] = scale_rows(head_out, hg_ref[...]).astype(jnp.bfloat16)


def attention_call(y, heads, query_gain, key_gain, weight_two, head_gain):
    rows = y.shape[0]
    half, vsize = query_gain.shape[0], head_gain.shape[0]
    block = math.gcd(rows, 256)
    small = lambda h, i: (0, 0)
    return pl.pallas_call(
        lambda *refs: attention_kernel(half, *refs),
        out_shape=jax.ShapeDtypeStruct((rows, heads * vsize), jnp.bfloat16),
        grid=(heads, rows // block),
        in_specs=[
            pl.BlockSpec((block, 2 * half), lambda h, i: (i, h)),
            pl.BlockSpec((rows, 2 * half), lambda h, i: (0, heads + h)),
            pl.BlockSpec((rows, vsize), lambda h, i: (0, 2 * heads + h)),
            pl.BlockSpec((1, 2 * half), small),
            pl.BlockSpec((1, 2 * half), small),
            pl.BlockSpec((1, 1, vsize), lambda h, i: (h, 0, 0)),
            pl.BlockSpec((1, vsize), small),
        ],
        out_specs=pl.BlockSpec((block, vsize), lambda h, i: (i, h)),
        scratch_shapes=[
            pltpu.VMEM((rows, 2 * half), jnp.bfloat16),
            pltpu.VMEM((rows, vsize), jnp.bfloat16),
        ],
        compiler_params=pltpu.CompilerParams(vmem_limit_bytes=40 * 2**20),
        cost_estimate=pl.CostEstimate(
            flops=heads * rows * rows * 8 * half * 2,
            bytes_accessed=rows * heads * vsize * 14,
            transcendentals=2 * heads * rows * rows,
        ),
    )(
        y,
        y,
        y,
        jnp.tile(query_gain, 2)[None],
        jnp.tile(key_gain, 2)[None],
        jnp.broadcast_to(weight_two[:, None, None], (heads, 1, vsize)),
        head_gain[None],
    )


def column_parts(weights, parts):
    rows = weights[0].shape[0]
    pieces = [w.reshape(rows, parts, w.shape[1] // parts) for w in weights]
    return jnp.transpose(jnp.concatenate(pieces, axis=2), (1, 0, 2))


def remote(source, target, send, recv, where):
    return pltpu.make_async_remote_copy(
        src_ref=source,
        dst_ref=target,
        send_sem=send,
        recv_sem=recv,
        device_id=where,
        device_id_type=pl.DeviceIdType.MESH,
    )


def meet(places):
    barrier = pltpu.get_barrier_semaphore()
    for where in places:
        pl.semaphore_signal(
            barrier, inc=1, device_id=where, device_id_type=pl.DeviceIdType.MESH
        )
    pl.semaphore_wait(barrier, len(places))


def gather_kernel(
    n, w_ref, t_ref, w_all, t_all, own, z_send, z_recv, f_send, f_recv, g_send, g_recv,
    t_send, t_recv, p_send, p_recv,
):
    z, f, c = lax.axis_index("sp"), lax.axis_index("fs"), lax.axis_index("tp")
    beside, above = f + 1 - 2 * (f % 2), f + 2 - 4 * (f // 2)
    rows = t_ref.shape[0]
    near = sorted(range(1, n), key=lambda d: min(d, n - d))
    meet(
        [{"sp": (z + d) % n} for d in near] + [{"fs": beside}, {"fs": above}, {"tp": 1 - c}]
    )

    def place(s):
        return t_all.at[c, pl.ds(pl.multiple_of(s * rows, rows), rows)]

    flights = []

    def go(copy):
        copy.start()
        flights.append(copy)
        return copy

    across = {
        d: go(
            remote(
                w_ref.at[(z + d) % n], w_all.at[z, f], z_send.at[d], z_recv.at[d], {"sp": (z + d) % n}
            )
        )
        for d in near
    }
    side = {}

    def spread(d, source):
        s = (z + n - d) % n
        for i, to in enumerate((beside, above)):
            side[i, d] = go(
                remote(source, w_all.at[s, f], f_send.at[i, d], f_recv.at[i, d], {"fs": to})
            )

    def pass_on(d):
        s = (z + n - d) % n
        i = d % 2
        side[i, d].wait_recv()
        held, to = (beside, above) if i == 0 else (above, beside)
        go(remote(w_all.at[s, held], w_all.at[s, held], g_send.at[d], g_recv.at[d], {"fs": to}))

    spread(0, w_ref.at[z])
    def along(source, s, step):
        return remote(source, place(s), t_send.at[(step + 1) // 2, s], t_recv.at[s], {"sp": z + step})

    def aside(source, s):
        return remote(source, place(s), p_send.at[s], p_recv.at[s], {"tp": 1 - c})

    @pl.when(z + 1 < n)
    def _():
        along(t_ref, z, 1).start()

    @pl.when(z > 0)
    def _():
        along(t_ref, z, -1).start()

    aside(t_ref, z).start()
    mine = [
        pltpu.make_async_copy(w_ref.at[z], w_all.at[z, f], own.at[0]),
        pltpu.make_async_copy(t_ref, place(z), own.at[1]),
    ]
    for copy in mine:
        copy.start()
    last = 0
    for d in near:
        across[d].wait_recv()
        spread(d, w_all.at[(z + n - d) % n, f])
        pass_on(last)
        last = d
    pass_on(last)
    for k in range(1, n):
        for step in (1, -1):
            s = z - step * k

            @pl.when(jnp.logical_and(s >= 0, s < n))
            def _(s=s, step=step):
                along(place(s), s, step).wait_recv()

                @pl.when(jnp.logical_and(z + step >= 0, z + step < n))
                def _():
                    along(place(s), s, step).start()

                aside(place(s), s).start()

    for k in range(n):
        for step in (1, -1) if k else (1,):
            s = z - step * k

            @pl.when(jnp.logical_and(s >= 0, s < n))
            def _(s=s, step=step, k=k):
                for way in (step,) if k else (1, -1):
                    @pl.when(jnp.logical_and(z + way >= 0, z + way < n))
                    def _(way=way):
                        along(place(s), s, way).wait_send()

                aside(place(s), s).wait_send()
                aside(place(s), s).wait_recv()

    waited = set(map(id, across.values()))
    waited |= {id(side[d % 2, d]) for d in range(n)}
    for copy in flights:
        copy.wait_send()
        if id(copy) not in waited:
            copy.wait_recv()
    for copy in mine:
        copy.wait()


def gather_all(packed, tokens):
    n, rows, columns = packed.shape
    fs, tp = lax.axis_size("fs"), lax.axis_size("tp")
    dma = pltpu.SemaphoreType.DMA
    return pl.pallas_call(
        lambda *refs: gather_kernel(n, *refs),
        out_shape=(
            jax.ShapeDtypeStruct((n, fs, rows, columns), packed.dtype),
            jax.ShapeDtypeStruct((tp, n * tokens.shape[0], tokens.shape[1]), tokens.dtype),
        ),
        in_specs=[pl.BlockSpec(memory_space=pltpu.VMEM)] * 2,
        out_specs=(pl.BlockSpec(memory_space=pl.ANY),) * 2,
        scratch_shapes=[
            dma((2,)), dma((n,)), dma((n,)), dma((2, n)), dma((2, n)), dma((n,)), dma((n,)),
            dma((2, n)), dma((n,)), dma((n,)), dma((n,)),
        ],
        compiler_params=pltpu.CompilerParams(collective_id=1, has_side_effects=True),
    )(packed, tokens)


def reduce_kernel(n, p_ref, out_ref, twin, pair, others, a_send, a_recv, b_send, b_recv):
    z, c = lax.axis_index("sp"), lax.axis_index("tp")
    near = sorted(range(1, n), key=lambda d: -min(d, n - d))
    meet([{"sp": (z + d) % n} for d in near] + [{"tp": 1 - c}])
    rows = out_ref.shape[0]
    tile = math.gcd(rows, 32)
    swaps = {}
    for d in near + [0]:
        s = (z + d) % n
        swaps[d] = remote(
            p_ref.at[1 - c, s], twin.at[d], a_send.at[d], a_recv.at[d], {"tp": 1 - c}
        )
        swaps[d].start()
    sends = {}
    for d in near + [0]:
        s = (z + d) % n
        swaps[d].wait_recv()

        def add(i, unused, s=s, d=d):
            at = pl.ds(pl.multiple_of(i * tile, tile), tile)
            total = p_ref[c, s, at, :].astype(jnp.float32) + twin[d, at, :].astype(jnp.float32)
            pair[d, at, :] = total.astype(jnp.bfloat16)
            return unused

        lax.fori_loop(0, rows // tile, add, 0)
        if d:
            sends[d] = remote(
                pair.at[d], others.at[d - 1], b_send.at[d - 1], b_recv.at[d - 1], {"sp": s}
            )
            sends[d].start()
    for d in near:
        sends[d].wait_recv()

    def finish(i, unused):
        at = pl.ds(pl.multiple_of(i * tile, tile), tile)
        total = pair[0, at, :].astype(jnp.float32)
        for d in range(1, n):
            total += others[d - 1, at, :].astype(jnp.float32)
        out_ref[at, :] = total.astype(jnp.bfloat16)
        return unused

    lax.fori_loop(0, rows // tile, finish, 0)
    for d in near + [0]:
        swaps[d].wait_send()
    for d in near:
        sends[d].wait_send()


def reduce_all(partial):
    tp, n, rows, width = partial.shape
    dma = pltpu.SemaphoreType.DMA
    return pl.pallas_call(
        lambda *refs: reduce_kernel(n, *refs),
        out_shape=jax.ShapeDtypeStruct((rows, width), partial.dtype),
        in_specs=[pl.BlockSpec(memory_space=pltpu.VMEM)],
        out_specs=pl.BlockSpec(memory_space=pltpu.VMEM),
        scratch_shapes=[
            pltpu.VMEM((n, rows, width), partial.dtype),
            pltpu.VMEM((n, rows, width), partial.dtype),
            pltpu.VMEM((n - 1, rows, width), partial.dtype),
            dma((n,)), dma((n,)), dma((n - 1,)), dma((n - 1,)),
        ],
        compiler_params=pltpu.CompilerParams(
            collective_id=2, has_side_effects=True, vmem_limit_bytes=48 * 2**20
        ),
    )(partial)


def split_device(
    inputs,
    norm_gain,
    query_weight,
    key_weight,
    value_weight,
    query_gain,
    key_gain,
    mix_lambda,
    head_gain,
    post_gate_weight,
    pre_gate_weight,
    inner_weight,
    conv_taps,
    attn_out_weight,
    conv_out_weight,
):
    sp, tp = lax.axis_size("sp"), lax.axis_size("tp")
    tokens = inputs[0]
    place = lax.axis_index("tp") * sp + lax.axis_index("sp")
    vsize = head_gain.shape[0]
    heads = value_weight.shape[1] // vsize // sp
    channels = post_gate_weight.shape[1] // sp
    weight_two = lax.dynamic_slice_in_dim(mix_lambda, place * heads, heads)
    taps = lax.dynamic_slice_in_dim(conv_taps, place * channels, channels, 1)
    packed = column_parts(
        (
            query_weight,
            key_weight,
            value_weight,
            post_gate_weight,
            pre_gate_weight,
            inner_weight,
            attn_out_weight,
            conv_out_weight,
        ),
        sp,
    )
    every, both = gather_all(packed, tokens)
    every = every.reshape(-1, packed.shape[2])
    cut = 3 * heads * vsize + 3 * channels
    into, outof = every[:, :cut], every[:, cut:]
    whole = jnp.concatenate([both[i] for i in range(tp)], axis=1)
    normed = scale_rows(whole.astype(jnp.float32), norm_gain).astype(jnp.bfloat16)
    y = jnp.dot(normed, into, preferred_element_type=jnp.float32)
    attn_hidden = attention_call(y, heads, query_gain, key_gain, weight_two, head_gain)
    span = 3 * heads * vsize
    post, pre_gate, inner = [
        y[:, span + i * channels : span + (i + 1) * channels] for i in range(3)
    ]
    post_wide = lax.optimization_barrier(post.astype(jnp.bfloat16)).astype(jnp.float32)
    signal = lax.optimization_barrier((pre_gate * inner).astype(jnp.bfloat16))
    shifted = jnp.pad(signal.astype(jnp.float32), ((1, 1), (0, 0)))
    filtered = taps[0] * shifted[:-2] + taps[1] * shifted[1:-1] + taps[2] * shifted[2:]
    conv_hidden = (post_wide * filtered).astype(jnp.bfloat16)
    hidden = jnp.concatenate([attn_hidden, conv_hidden], axis=1)
    width = hidden.shape[1]
    hidden = hidden.reshape(sp, tp, -1, width).transpose(1, 0, 2, 3).reshape(-1, width)
    partial = lax.dot_general(
        hidden, outof, (((1,), (1,)), ((), ())), preferred_element_type=jnp.float32
    ).astype(jnp.bfloat16)
    summed = reduce_all(partial.reshape(tp, sp, -1, partial.shape[1]))
    return summed[None]


def per_device(
    inputs,
    norm_gain,
    query_weight,
    key_weight,
    value_weight,
    query_gain,
    key_gain,
    mix_lambda,
    head_gain,
    post_gate_weight,
    pre_gate_weight,
    inner_weight,
    conv_taps,
    attn_out_weight,
    conv_out_weight,
):
    tokens = inputs[0]
    whole = lax.all_gather(tokens, "tp", axis=1, tiled=True)
    normed = scale_rows(whole.astype(jnp.float32), norm_gain).astype(jnp.bfloat16)
    heads_dev = value_weight.shape[1] // head_gain.shape[0]
    channels = post_gate_weight.shape[1]
    tp_index = lax.axis_index("tp")
    weight_two = lax.dynamic_slice_in_dim(mix_lambda, tp_index * heads_dev, heads_dev)
    taps = lax.dynamic_slice_in_dim(conv_taps, tp_index * channels, channels, 1)
    every_full = (
        lax.all_gather(query_weight, ("sp", "fs"), axis=0, tiled=True),
        lax.all_gather(key_weight, ("sp", "fs"), axis=0, tiled=True),
        lax.all_gather(value_weight, ("sp", "fs"), axis=0, tiled=True),
        lax.all_gather(post_gate_weight, ("sp", "fs"), axis=0, tiled=True),
        lax.all_gather(pre_gate_weight, ("sp", "fs"), axis=0, tiled=True),
        lax.all_gather(inner_weight, ("sp", "fs"), axis=0, tiled=True),
        lax.all_gather(attn_out_weight, ("sp", "fs"), axis=0, tiled=True),
        lax.all_gather(conv_out_weight, ("sp", "fs"), axis=0, tiled=True),
    )
    query, key, value_proj, post, pre_gate, inner, attn_out_full, conv_out_full = project_all(
        normed, every_full[0:3] + every_full[3:6] + every_full[6:8], 6
    )
    attn_hidden = attention_branch(
        query, key, value_proj.astype(jnp.bfloat16), weight_two, query_gain, key_gain, head_gain
    )
    post_mid = post.astype(jnp.bfloat16)
    post_wide = lax.optimization_barrier(post_mid).astype(jnp.float32)
    signal = (pre_gate * inner).astype(jnp.bfloat16)
    padded = padded_2(signal, (("sp", 0),), 1)
    shifted = lax.optimization_barrier(padded).astype(jnp.float32)
    filtered = taps[0] * shifted[:-2] + taps[1] * shifted[1:-1] + taps[2] * shifted[2:]
    conv_hidden = (post_wide * filtered).astype(jnp.bfloat16)
    contract = (((1,), (1,)), ((), ()))
    summed = lax.psum_scatter(
        (
            lax.dot_general(
                attn_hidden, attn_out_full, contract, preferred_element_type=jnp.float32
            )
            + lax.dot_general(
                conv_hidden, conv_out_full, contract, preferred_element_type=jnp.float32
            )
        ).astype(jnp.bfloat16),
        "tp",
        scatter_dimension=0,
        tiled=True,
    )
    return summed[None]


def solution(mesh):
    placed = (
        P("fs", "sp", "tp"),
        P(),
        P(("sp", "fs"), "tp"),
        P(("sp", "fs"), "tp"),
        P(("sp", "fs"), "tp"),
        P(),
        P(),
        P(),
        P(),
        P(("sp", "fs"), "tp"),
        P(("sp", "fs"), "tp"),
        P(("sp", "fs"), "tp"),
        P(),
        P(("sp", "fs"), "tp"),
        P(("sp", "fs"), "tp"),
    )
    sp, tp = mesh.shape["sp"], mesh.shape["tp"]

    def program(*args):
        heads = args[7].shape[0]
        channels = args[12].shape[1]
        splits = tp == 2 and mesh.shape["fs"] == 4 and sp > 1 and heads % (sp * tp) == 0
        splits = splits and channels % (sp * tp * 128) == 0
        return shard(split_device if splits else per_device)(*args)

    shard = lambda body: jax.shard_map(
        body,
        mesh=mesh,
        in_specs=placed,
        out_specs=P("fs", ("sp", "tp"), None),
        check_vma=False,
    )

    return program
```
